32 devices in a mesh: sp: 8 (over z, y), tp: 4 (over x, core).
Axes of the slice: x: 2, y: 2, z: 4, core: 2. Of those that a mesh axis runs over, the one named last changes fastest.
Arguments:
- mixer_input: bfloat16 [1024, 1024], P('sp', 'tp'), may hold values from -1800 to 1800
- time_step: float32 [2, 64], P(None, 'tp'), may hold values from 0 to 2, as said below
- damping: float32 [2, 1024, 64], P(None, 'sp', 'tp'), may hold values from 0 to 2
- input_map: bfloat16 [2, 2, 64, 64, 16], P(None, None, 'tp'), may hold values from -1 to 1
- readout: float32 [2, 2, 64, 16, 64], P(None, None, 'tp'), may hold values from -0.5 to 0.5
- skip_gain: float32 [1024], P('tp'), may hold values from -4 to 4
- out_gain: float32 [1024], P('tp'), may hold values from 0.1 to 1.9
- out_weight: bfloat16 [1024, 2048], replicated, may hold values from -0.1875 to 0.1875
- residual: bfloat16 [1024, 2048], P(('sp', 'tp')), may hold values from -6 to 6
- channel_gain: float32 [2048], replicated, may hold values from 0.1 to 1.9
- value_weight: bfloat16 [2048, 6144], P('sp', 'tp'), may hold values from -0.125 to 0.125
- gate_weight: bfloat16 [2048, 6144], P('sp', 'tp'), may hold values from -0.125 to 0.125
- value_taps: float32 [3, 6144], P(None, 'tp'), may hold values from -3 to 3
- gate_taps: float32 [3, 6144], P(None, 'tp'), may hold values from -3 to 3
- down_weight: bfloat16 [6144, 2048], P('tp', 'sp'), may hold values from -0.078125 to 0.078125
Outputs:
- output: bfloat16 [1024, 2048], P(('sp', 'tp'))
The draws below stay inside these ranges and needn't reach their ends.
Inputs may be any that keep to these rules, and one draw needn't show every extreme that they name: `time_step`: positive.
All inputs are finite; a program needn't handle non-finite values.
Results may differ from the reference program's by a relative error of at most 0.017.
Values may be sent and summed in bfloat16 or wider, within the bound.
A program may use at most 128 MiB of HBM per device.

```python
import math
import jax
import jax.numpy as jnp
from jax import lax

D = 2048
DS = 1024
GROUP = 16
STATE = 64
FF = 6144
TOK_DEV = 128
G = 64
TOKEN_POSITIONS = 1024
N_TP = 4


def draw_mixer_input(key, part):
    split_random_keys = jax.random.split(key, 3)
    column_pos = jnp.arange(DS, dtype=jnp.float32) / DS
    spread = math.log(10.0)
    noise = jnp.clip(jax.random.normal(split_random_keys[0], (TOKEN_POSITIONS, DS), jnp.float32), -5.0, 5.0)
    row_scale = jnp.exp(jax.random.uniform(split_random_keys[2], (TOKEN_POSITIONS, 1), jnp.float32, 0.0, spread))
    column_scale = jnp.exp(spread * column_pos)[None, :]
    return (noise * row_scale * column_scale).astype(jnp.float32).astype(jnp.bfloat16)


def draw_time_step(key, part):
    split_random_keys = jax.random.split(key, 3)
    group_count = DS // GROUP
    chance = jax.random.randint(split_random_keys[0], (2, group_count), 0, 16)
    quick = chance < 8
    quick_rate = jnp.exp(jax.random.uniform(split_random_keys[1], (2, group_count), jnp.float32, math.log(5.0 / TOK_DEV), math.log(16.0 / TOK_DEV)))
    slow_rate = jnp.exp(jax.random.uniform(split_random_keys[2], (2, group_count), jnp.float32, math.log(0.2 / TOKEN_POSITIONS), math.log(1.0 / TOKEN_POSITIONS)))
    return 2.0 * jnp.where(quick, quick_rate, slow_rate)


def draw_damping(key, part):
    split_random_keys = jax.random.split(key, 4)
    group_count = DS // GROUP
    blocks = TOKEN_POSITIONS // TOK_DEV
    baseline_rate = jnp.exp(jax.random.uniform(split_random_keys[0], (2, 1, group_count), jnp.float32, math.log(0.1), math.log(0.4))) / TOKEN_POSITIONS
    multiplier = jnp.exp(jax.random.uniform(split_random_keys[1], (2, blocks, group_count), jnp.float32, 0.0, math.log(4.0)))
    multiplier = jnp.repeat(multiplier, TOK_DEV, axis=1)
    spike_locations = jax.random.randint(split_random_keys[2], (2, 1, group_count, 3), 0, TOKEN_POSITIONS)
    dropped_fraction = jax.random.uniform(split_random_keys[3], (2, 1, group_count, 3), jnp.float32, 0.2, 0.33)
    token_position = jnp.arange(TOKEN_POSITIONS, dtype=jnp.int32)[None, :, None, None]
    sudden_spike = jnp.sum(jnp.where(token_position == spike_locations, -jnp.log1p(-dropped_fraction), 0.0), axis=3)
    return (baseline_rate * multiplier + sudden_spike).astype(jnp.float32)


def block_levels(rng, dims, cuts, smallest, top_value):
    level, own = 1.0, jax.random.fold_in(rng, 6)
    for axis_at, shards_of in cuts:
        draws = jnp.exp(jax.random.uniform(jax.random.fold_in(own, axis_at), (shards_of,), jnp.float32, smallest / len(cuts), top_value / len(cuts)))
        level = level * jnp.repeat(draws, dims[axis_at] // shards_of).reshape([-1 if axis == axis_at else 1 for axis in range(len(dims))])
    return level


def normal_values(rng, extent, scale, limit, cuts=(), kind=jnp.bfloat16):
    level = block_levels(rng, extent, cuts, -0.22, 0.18) if cuts else 1.0
    array = jax.random.normal(rng, extent, jnp.float32) * scale * level
    return jnp.minimum(jnp.maximum(array, -limit), limit).astype(kind)


def setup_inputs(seed: int = 0) -> dict:
    key_of = jax.random.split(jax.random.key(seed), 16)
    mixer_input = draw_mixer_input(jax.random.fold_in(key_of[15], 71), 0)
    time_step = draw_time_step(jax.random.fold_in(key_of[15], 71), 0)
    damping = draw_damping(jax.random.fold_in(key_of[15], 71), 0)
    input_map = normal_values(key_of[3], (2, 2, G, STATE, GROUP), (2 * GROUP) ** -0.5, 1.0, ((2, 4),))
    readout = normal_values(key_of[4], (2, 2, G, GROUP, STATE), (2 * STATE) ** -0.5, 0.5, ((2, 4),), jnp.float32)
    skip_gain = normal_values(key_of[5], (DS,), 1.0, 4.0, ((0, 4),), jnp.float32)
    out_gain = jnp.clip(1.0 + 0.18 * jax.random.normal(key_of[6], (DS,), jnp.float32), 0.1, 1.9)
    out_weight = normal_values(key_of[7], (DS, D), DS ** -0.5, 0.1875)
    residual = normal_values(key_of[8], (TOKEN_POSITIONS, D), 1.0, 6.0, ((0, 32),))
    channel_gain = jnp.clip(1.0 + 0.18 * jax.random.normal(key_of[9], (D,), jnp.float32), 0.1, 1.9)
    value_weight = normal_values(key_of[10], (D, FF), D ** -0.5, 0.125, ((0, 8), (1, 4)))
    gate_weight = normal_values(key_of[11], (D, FF), D ** -0.5, 0.125, ((0, 8), (1, 4)))
    value_taps = normal_values(key_of[12], (3, FF), 0.577, 3.0, ((1, 4),), jnp.float32)
    gate_taps = normal_values(key_of[13], (3, FF), 0.577, 3.0, ((1, 4),), jnp.float32)
    down_weight = normal_values(key_of[14], (FF, D), FF ** -0.5, 0.078125, ((0, 4), (1, 8)))
    return dict(mixer_input=mixer_input, time_step=time_step, damping=damping, input_map=input_map, readout=readout, skip_gain=skip_gain, out_gain=out_gain, out_weight=out_weight, residual=residual, channel_gain=channel_gain, value_weight=value_weight, gate_weight=gate_weight, value_taps=value_taps, gate_taps=gate_taps, down_weight=down_weight)


norm_eps = 1e-06
highest = lax.Precision.HIGHEST

def combine(earlier, latter):
    prod_real = latter[0] * earlier[0] - latter[1] * earlier[1]
    prod_imag = latter[0] * earlier[1] + latter[1] * earlier[0]
    sum_real = latter[0] * earlier[2] - latter[1] * earlier[3] + latter[2]
    sum_imag = latter[0] * earlier[3] + latter[1] * earlier[2] + latter[3]
    return (prod_real, prod_imag, sum_real, sum_imag)

def group_mixer(operands):
    group_input, step_pair, damp_pair, in_maps, out_maps = operands
    states = in_maps.shape[2]
    frequency = math.pi * jnp.arange(states, dtype=jnp.float32)
    result = jnp.zeros(group_input.shape, jnp.float32)
    for direction in range(2):
        step_size = step_pair[direction]
        rotation = step_size * frequency
        magnitude = jnp.exp(-0.5 * step_size - damp_pair[direction])[:, None]
        decay_real = magnitude * jnp.cos(rotation)[None, :]
        decay_imag = magnitude * jnp.sin(rotation)[None, :]
        in_scale = jnp.sqrt(-jnp.expm1(-step_size))
        drive_real = jnp.dot(group_input, in_maps[direction, 0].T, preferred_element_type=jnp.float32) * in_scale
        drive_imag = jnp.dot(group_input, in_maps[direction, 1].T, preferred_element_type=jnp.float32) * in_scale
        scanned = lax.associative_scan(combine, (decay_real, decay_imag, drive_real, drive_imag), reverse=direction == 1, axis=0)
        result = result + jnp.dot(scanned[2], out_maps[direction, 0].T, precision=highest)
        result = result - jnp.dot(scanned[3], out_maps[direction, 1].T, precision=highest)
    return result

def shifted_sum(values, tap_rows):
    widened = jnp.pad(values.astype(jnp.float32), ((1, 1), (0, 0)))
    return tap_rows[0] * widened[:-2] + tap_rows[1] * widened[1:-1] + tap_rows[2] * widened[2:]

def reference(mixer_input, time_step, damping, input_map, readout, skip_gain, out_gain, out_weight, residual, channel_gain, value_weight, gate_weight, value_taps, gate_taps, down_weight):
    tokens, channels = mixer_input.shape
    group_count = time_step.shape[1]
    group_width = channels // group_count
    grouped = jnp.transpose(mixer_input.reshape(tokens, group_count, group_width), (1, 0, 2))
    per_group = lax.map(group_mixer, (grouped, time_step.T, jnp.transpose(damping, (2, 0, 1)), jnp.moveaxis(input_map, 2, 0), jnp.moveaxis(readout, 2, 0)))
    mixed_y = jnp.transpose(per_group, (1, 0, 2)).reshape(tokens, channels) + skip_gain[None, :] * mixer_input.astype(jnp.float32)
    inverse = lax.rsqrt(lax.optimization_barrier(jnp.mean(mixed_y * mixed_y, axis=1, keepdims=True)) + norm_eps)
    normed_mix = (mixed_y * inverse * out_gain[None, :]).astype(jnp.bfloat16)
    mixed_rows = jnp.dot(normed_mix, out_weight, preferred_element_type=jnp.float32)
    hidden_state = (residual.astype(jnp.float32) + mixed_rows).astype(jnp.bfloat16)
    state_wide = hidden_state.astype(jnp.float32)
    scale_rows = lax.rsqrt(lax.optimization_barrier(jnp.mean(state_wide * state_wide, axis=1, keepdims=True)) + norm_eps)
    normed = (state_wide * scale_rows * channel_gain[None, :]).astype(jnp.bfloat16)
    value_up = jnp.dot(normed, value_weight, preferred_element_type=jnp.float32).astype(jnp.bfloat16)
    gate_up = jnp.dot(normed, gate_weight, preferred_element_type=jnp.float32).astype(jnp.bfloat16)
    value_conv = shifted_sum(value_up, value_taps)
    gate_conv = shifted_sum(gate_up, gate_taps)
    hidden = (value_conv * jax.nn.silu(gate_conv)).astype(jnp.bfloat16)
    block_width = FF // N_TP
    summed = jnp.zeros((tokens, out_weight.shape[1]), jnp.float32)
    for part_index in range(N_TP):
        first_col = part_index * block_width
        partial_value = jnp.dot(hidden[:, first_col:first_col + block_width], down_weight[first_col:first_col + block_width], preferred_element_type=jnp.float32)
        rounded = lax.optimization_barrier(partial_value.astype(jnp.bfloat16))
        summed = summed + rounded.astype(jnp.float32)
    return (state_wide + summed).astype(jnp.bfloat16)
```

```python
import math

import jax
import jax.numpy as jnp
from jax import lax
from jax.sharding import PartitionSpec as P

norm_eps = 1e-06
highest = lax.Precision.HIGHEST


def turns(step_size, count):
    coarse = jnp.round(step_size * 1024.0) / 1024.0
    whole = coarse * count
    whole = whole - 2.0 * jnp.floor(whole * 0.5)
    return whole + (step_size - coarse) * count


def mixer(mixer_input, time_step, damping, input_map, readout, skip_gain):
    rows = mixer_input.shape[0]
    groups = time_step.shape[1]
    states, width = input_map.shape[3], input_map.shape[4]
    count, mine = lax.axis_size("sp"), lax.axis_index("sp")
    at = jnp.arange(rows)
    lower = at[:, None] >= at[None, :]
    reach = jnp.stack((lower, lower.T))
    log_decay = -0.5 * time_step[:, None, :] - damping
    log_sum = jnp.einsum("ktu,kug->kgt", reach.astype(jnp.float32), log_decay, precision=highest)
    weights = jnp.where(
        reach[:, None],
        jnp.exp(jnp.minimum(log_sum[:, :, :, None] - log_sum[:, :, None, :], 0.0)),
        0.0,
    )
    number = jnp.arange(states, dtype=jnp.float32)
    dt = time_step[:, :, None, None]
    angle = math.pi * turns(dt, number[None, :] * at.astype(jnp.float32)[:, None])
    sign = jnp.array([1.0, -1.0], jnp.float32)[:, None, None, None]
    cos, sin = jnp.cos(angle), jnp.sin(angle) * sign
    grouped = mixer_input.reshape(rows, groups, width)
    drive = jnp.einsum("tgh,kpgnh->kpgtn", grouped, input_map, preferred_element_type=jnp.float32)
    drive = drive * jnp.sqrt(-jnp.expm1(-time_step))[:, None, :, None, None]
    rotated = jnp.concatenate(
        (cos * drive[:, 0] + sin * drive[:, 1], cos * drive[:, 1] - sin * drive[:, 0]), axis=3
    )
    local = jnp.einsum("kgts,kgsn->kgtn", weights, rotated, precision=highest)
    ends = jnp.stack((local[0, :, -1], local[1, :, 0]))
    totals = jnp.stack((log_sum[0, :, -1], log_sum[1, :, 0]))
    packed = jnp.concatenate((ends, jnp.repeat(totals[:, :, None], 128, axis=2)), axis=2)
    every = lax.all_gather(packed, "sp")
    end_all, total_all = every[..., : 2 * states], every[..., 2 * states]
    index = jnp.arange(count)
    away = jnp.stack((mine - index, index - mine), axis=1)
    lo = jnp.minimum(index, mine)[:, None]
    hi = jnp.maximum(index, mine)[:, None]
    between = ((index[None, :] > lo) & (index[None, :] < hi)).astype(jnp.float32)
    span = jnp.einsum("ji,ikg->jkg", between, total_all, precision=highest)
    factor = jnp.where(away[:, :, None] > 0, jnp.exp(span), 0.0)
    block_turn = turns(time_step[:, :, None], number * rows)
    hop = jnp.abs(mine - index).astype(jnp.float32)[:, None, None, None] * block_turn
    hop = math.pi * (hop - 2.0 * jnp.floor(hop * 0.5))
    hop_cos, hop_sin = jnp.cos(hop) * factor[..., None], jnp.sin(hop) * factor[..., None]
    end_re, end_im = end_all[..., :states], end_all[..., states:]
    carry = jnp.concatenate(
        (
            jnp.sum(hop_cos * end_re - hop_sin * end_im, axis=0),
            jnp.sum(hop_cos * end_im + hop_sin * end_re, axis=0),
        ),
        axis=2,
    )
    local = local + jnp.exp(log_sum)[..., None] * carry[:, :, None, :]
    re, im = local[..., :states], local[..., states:]
    state = jnp.concatenate((cos * re - sin * im, cos * im + sin * re), axis=3)
    out_map = jnp.concatenate((readout[:, 0], -readout[:, 1]), axis=3)
    mixed = jnp.einsum("kgtn,kghn->tgh", state, out_map, precision=highest)
    return mixed.reshape(rows, groups * width) + skip_gain[None, :] * mixer_input.astype(
        jnp.float32
    )


def body(
    mixer_input,
    time_step,
    damping,
    input_map,
    readout,
    skip_gain,
    out_gain,
    out_weight,
    residual,
    channel_gain,
    value_weight,
    gate_weight,
    value_taps,
    gate_taps,
    down_weight,
):
    count, mine = lax.axis_size("sp"), lax.axis_index("sp")
    depth, hidden_width = value_weight.shape
    part = hidden_width // count
    up_send = jnp.concatenate(
        (
            value_weight.reshape(depth, count, part).swapaxes(0, 1),
            gate_weight.reshape(depth, count, part).swapaxes(0, 1),
        ),
        axis=2,
    )
    up_all = lax.all_to_all(up_send, "sp", split_axis=0, concat_axis=0, tiled=True)
    up_all = up_all.reshape(count * depth, 2 * part)
    down_send = down_weight.reshape(count, part, down_weight.shape[1])
    down_all = lax.all_to_all(down_send, "sp", split_axis=0, concat_axis=0, tiled=True)
    gain = lax.all_gather(out_gain, "tp", axis=0, tiled=True)
    mixed_y = mixer(mixer_input, time_step, damping, input_map, readout, skip_gain)
    mixed_y = lax.all_to_all(mixed_y, "tp", split_axis=0, concat_axis=1, tiled=True)
    inverse = lax.rsqrt(jnp.mean(mixed_y * mixed_y, axis=1, keepdims=True) + norm_eps)
    normed_mix = (mixed_y * inverse * gain[None, :]).astype(jnp.bfloat16)
    mixed_rows = jnp.dot(normed_mix, out_weight, preferred_element_type=jnp.float32)
    hidden_state = (residual.astype(jnp.float32) + mixed_rows).astype(jnp.bfloat16)
    state_wide = hidden_state.astype(jnp.float32)
    scale_rows = lax.rsqrt(jnp.mean(state_wide * state_wide, axis=1, keepdims=True) + norm_eps)
    normed = (state_wide * scale_rows * channel_gain[None, :]).astype(jnp.bfloat16)
    rows_all = lax.all_gather(normed, ("sp", "tp"), axis=0, tiled=True)
    up = jnp.dot(rows_all, up_all, preferred_element_type=jnp.float32)
    up = up.astype(jnp.bfloat16).astype(jnp.float32)
    taps = jnp.concatenate(
        (
            lax.dynamic_slice_in_dim(value_taps, mine * part, part, axis=1),
            lax.dynamic_slice_in_dim(gate_taps, mine * part, part, axis=1),
        ),
        axis=1,
    )
    padded = jnp.pad(up, ((1, 1), (0, 0)))
    convolved = taps[0] * padded[:-2] + taps[1] * padded[1:-1] + taps[2] * padded[2:]
    hidden = (convolved[:, :part] * jax.nn.silu(convolved[:, part:])).astype(jnp.bfloat16)
    partial = jnp.einsum("tf,sfd->tsd", hidden, down_all, preferred_element_type=jnp.float32)
    partial = partial.astype(jnp.bfloat16).reshape(hidden.shape[0], -1)
    summed = lax.psum_scatter(partial, ("sp", "tp"), scatter_dimension=0, tiled=True)
    return (state_wide + summed.astype(jnp.float32)).astype(jnp.bfloat16)


def solution(mesh):
    in_specs = (
        P("sp", "tp"),
        P(None, "tp"),
        P(None, "sp", "tp"),
        P(None, None, "tp", None, None),
        P(None, None, "tp", None, None),
        P("tp"),
        P("tp"),
        P(),
        P(("sp", "tp"), None),
        P(),
        P("sp", "tp"),
        P("sp", "tp"),
        P(None, "tp"),
        P(None, "tp"),
        P("tp", "sp"),
    )
    out_specs = P(("sp", "tp"), None)
    return jax.shard_map(body, mesh=mesh, in_specs=in_specs, out_specs=out_specs, check_vma=False)
```

```python
import math

import jax
import jax.numpy as jnp
from jax import lax
from jax.experimental import pallas as pl
from jax.experimental.pallas import tpu as pltpu
from jax.sharding import PartitionSpec as P

norm_eps = 1e-06
highest = lax.Precision.HIGHEST
mesh_ids = pl.DeviceIdType.MESH


def carry_kernel(count, own_ref, all_ref, local_sem, send_sem, recv_sem):
    sp, tp = lax.axis_index("sp"), lax.axis_index("tp")
    barrier = pltpu.get_barrier_semaphore()
    for offset in range(1, count):
        peer = lax.rem(sp + offset, count)
        pl.semaphore_signal(barrier, inc=1, device_id=(peer, tp), device_id_type=mesh_ids)
    pl.semaphore_wait(barrier, count - 1)
    keep = pltpu.make_async_copy(own_ref, all_ref.at[sp], local_sem)
    keep.start()
    copies = []
    for offset in range(1, count):
        peer = lax.rem(sp + offset, count)
        copy = pltpu.make_async_remote_copy(
            src_ref=own_ref,
            dst_ref=all_ref.at[sp],
            send_sem=send_sem.at[offset],
            recv_sem=recv_sem.at[offset],
            device_id=(peer, tp),
            device_id_type=mesh_ids,
        )
        copy.start()
        copies.append(copy)
    keep.wait()
    for copy in copies:
        copy.wait()


def gather_ends(packed, count):
    vmem = pl.BlockSpec(memory_space=pltpu.VMEM)
    return pl.pallas_call(
        lambda *refs: carry_kernel(count, *refs),
        name="gather_ends",
        out_shape=jax.ShapeDtypeStruct((count,) + packed.shape, packed.dtype),
        in_specs=[vmem],
        out_specs=vmem,
        scratch_shapes=[
            pltpu.SemaphoreType.DMA,
            pltpu.SemaphoreType.DMA((count,)),
            pltpu.SemaphoreType.DMA((count,)),
        ],
        compiler_params=pltpu.CompilerParams(collective_id=0, has_side_effects=True),
    )(packed)


gather_orders = (("z", "y", "x", "c"), ("x", "y", "z", "c"))
sum_orders = (("c", "x", "y", "z"), ("c", "z", "y", "x"))
axes = ("z", "y", "x", "c")


def channel_kernel(sizes, *refs):
    normed_ref, hidden_state_ref, up_ref, down_ref, taps_ref, out_ref = refs[:6]
    rows_all, up_rows, partial = refs[6:9]
    landing = refs[9:17]
    local_sem, send_sem, recv_sem = refs[17:20]
    rows, width = normed_ref.shape
    half = width // 2
    part = up_ref.shape[1] // 2
    sp, tp = lax.axis_index("sp"), lax.axis_index("tp")
    mine = {
        "z": sp // sizes["y"],
        "y": lax.rem(sp, sizes["y"]),
        "x": tp // sizes["c"],
        "c": lax.rem(tp, sizes["c"]),
    }

    def neighbour(axis, offset):
        at = dict(mine)
        at[axis] = lax.rem(mine[axis] + offset, sizes[axis])
        return at[axis], (at["z"] * sizes["y"] + at["y"], at["x"] * sizes["c"] + at["c"])

    barrier = pltpu.get_barrier_semaphore()
    greeted = 0
    for axis in axes:
        for offset in range(1, sizes[axis]):
            _, device = neighbour(axis, offset)
            pl.semaphore_signal(barrier, inc=1, device_id=device, device_id_type=mesh_ids)
            greeted += 1
    pl.semaphore_wait(barrier, greeted)

    keep = pltpu.make_async_copy(
        normed_ref, rows_all.at[mine["z"], mine["y"], mine["x"], mine["c"]], local_sem
    )
    keep.start()
    keep.wait()

    slot = 0
    pending = [[], []]
    for stage in range(4):
        for piece in range(2):
            axis = gather_orders[piece][stage]
            done = gather_orders[piece][:stage]
            for copy in pending[piece]:
                copy.wait()
            pending[piece] = []
            index = tuple(slice(None) if name in done else mine[name] for name in axes)
            block = rows_all.at[index + (slice(None), pl.ds(piece * half, half))]
            for offset in range(1, sizes[axis]):
                _, device = neighbour(axis, offset)
                copy = pltpu.make_async_remote_copy(
                    src_ref=block,
                    dst_ref=block,
                    send_sem=send_sem.at[slot],
                    recv_sem=recv_sem.at[slot],
                    device_id=device,
                    device_id_type=mesh_ids,
                )
                copy.start()
                pending[piece].append(copy)
                slot += 1
    for piece in range(2):
        for copy in pending[piece]:
            copy.wait()

    plane = sizes["y"] * sizes["x"] * sizes["c"] * rows
    total = plane * sizes["z"]
    edge = jnp.zeros((8, up_rows.shape[1]), jnp.float32)
    up_rows[pl.ds(0, 8), :] = edge
    up_rows[pl.ds(total + 8, 8), :] = edge

    def project(z, _):
        block = rows_all[z].reshape(plane, width)
        up = jnp.dot(block, up_ref[...], preferred_element_type=jnp.float32)
        start = pl.multiple_of(z * plane + 8, 8)
        up_rows[pl.ds(start, plane), :] = up.astype(jnp.bfloat16).astype(jnp.float32)
        return _

    lax.fori_loop(0, sizes["z"], project, 0)

    def mix(z, _):
        start = pl.multiple_of(z * plane, 8)
        window = up_rows[pl.ds(start, plane + 16), :]
        convolved = (
            taps_ref[0:1, :] * window[7 : plane + 7]
            + taps_ref[1:2, :] * window[8 : plane + 8]
            + taps_ref[2:3, :] * window[9 : plane + 9]
        )
        gate = convolved[:, part:]
        hidden = convolved[:, :part] * (gate / (1.0 + jnp.exp(-gate)))
        sums = jnp.dot(
            hidden.astype(jnp.bfloat16), down_ref[...], preferred_element_type=jnp.float32
        )
        partial[z] = sums.astype(jnp.bfloat16).reshape(partial.shape[1:])
        return _

    lax.fori_loop(0, sizes["z"], mix, 0)

    def start_sum(piece, stage, slot):
        axis = sum_orders[piece][stage]
        done = sum_orders[piece][:stage]
        started = []
        for offset in range(1, sizes[axis]):
            place, device = neighbour(axis, offset)
            index = tuple(
                place if name == axis else mine[name] if name in done else slice(None)
                for name in axes
            )
            copy = pltpu.make_async_remote_copy(
                src_ref=partial.at[index + (slice(None), pl.ds(piece * half, half))],
                dst_ref=landing[piece * 4 + stage].at[offset - 1],
                send_sem=send_sem.at[slot],
                recv_sem=recv_sem.at[slot],
                device_id=device,
                device_id_type=mesh_ids,
            )
            copy.start()
            started.append(copy)
            slot += 1
        return started, slot

    def add_landed(piece, stage):
        axis = sum_orders[piece][stage]
        done = sum_orders[piece][: stage + 1]
        land = landing[piece * 4 + stage]
        columns = pl.ds(piece * half, half)
        free = [name for name in axes if name not in done]

        def add(step, _):
            index, inner = [], ()
            for name in axes:
                if name in done:
                    index.append(mine[name])
                elif name == free[0]:
                    index.append(step)
                    inner = (step,)
                else:
                    index.append(slice(None))
            index = tuple(index) + (slice(None), columns)
            value = partial[index].astype(jnp.float32)
            for offset in range(1, sizes[axis]):
                value = value + land[(offset - 1,) + inner].astype(jnp.float32)
            if free:
                partial[index] = value.astype(jnp.bfloat16)
            else:
                out_ref[:, columns] = (
                    hidden_state_ref[:, columns].astype(jnp.float32) + value
                ).astype(jnp.bfloat16)
            return _

        if free:
            lax.fori_loop(0, sizes[free[0]], add, 0)
        else:
            add(0, 0)

    slot = send_sem.shape[0] // 2
    for stage in range(4):
        for piece in range(2):
            if stage:
                for copy in pending[piece]:
                    copy.wait()
                add_landed(piece, stage - 1)
            pending[piece], slot = start_sum(piece, stage, slot)
    for piece in range(2):
        for copy in pending[piece]:
            copy.wait()
        add_landed(piece, 3)


def channel_mixer(normed, hidden_state, up_all, down_all, taps, sp_count, tp_count):
    cores = 2
    across = tp_count // cores
    deep = math.gcd(across, sp_count)
    sizes = {"z": sp_count // deep, "y": deep, "x": across, "c": cores}
    rows, width = normed.shape
    half = width // 2
    grid = tuple(sizes[name] for name in axes)
    total = math.prod(grid) * rows
    landing = []
    for order in sum_orders:
        for stage in range(4):
            axis = order[stage]
            left = tuple(sizes[name] for name in axes if name not in order[: stage + 1])
            landing.append(
                pltpu.VMEM((max(sizes[axis] - 1, 1),) + left + (rows, half), jnp.bfloat16)
            )
    copies = 2 * 2 * sum(max(sizes[name] - 1, 0) for name in axes)
    vmem = pl.BlockSpec(memory_space=pltpu.VMEM)
    return pl.pallas_call(
        lambda *refs: channel_kernel(sizes, *refs),
        name="channel_mixer",
        out_shape=jax.ShapeDtypeStruct((rows, width), jnp.bfloat16),
        in_specs=[vmem] * 5,
        out_specs=vmem,
        scratch_shapes=[
            pltpu.VMEM(grid + (rows, width), jnp.bfloat16),
            pltpu.VMEM((total + 16, up_all.shape[1]), jnp.float32),
            pltpu.VMEM(grid + (rows, width), jnp.bfloat16),
            *landing,
            pltpu.SemaphoreType.DMA,
            pltpu.SemaphoreType.DMA((copies,)),
            pltpu.SemaphoreType.DMA((copies,)),
        ],
        compiler_params=pltpu.CompilerParams(
            collective_id=1, has_side_effects=True, vmem_limit_bytes=63 * 1024 * 1024
        ),
    )(normed, hidden_state, up_all, down_all, taps)


def turns(step_size, count):
    coarse = jnp.round(step_size * 1024.0) / 1024.0
    whole = coarse * count
    whole = whole - 2.0 * jnp.floor(whole * 0.5)
    return whole + (step_size - coarse) * count


def mixer(mixer_input, time_step, damping, input_map, readout, skip_gain):
    rows = mixer_input.shape[0]
    groups = time_step.shape[1]
    states, width = input_map.shape[3], input_map.shape[4]
    count, mine = lax.axis_size("sp"), lax.axis_index("sp")
    at = jnp.arange(rows)
    lower = at[:, None] >= at[None, :]
    reach = jnp.stack((lower, lower.T))
    log_decay = -0.5 * time_step[:, None, :] - damping
    log_sum = jnp.einsum("ktu,kug->kgt", reach.astype(jnp.float32), log_decay, precision=highest)
    weights = jnp.where(
        reach[:, None],
        jnp.exp(jnp.minimum(log_sum[:, :, :, None] - log_sum[:, :, None, :], 0.0)),
        0.0,
    )
    number = jnp.arange(states, dtype=jnp.float32)
    dt = time_step[:, :, None, None]
    angle = math.pi * turns(dt, number[None, :] * at.astype(jnp.float32)[:, None])
    sign = jnp.array([1.0, -1.0], jnp.float32)[:, None, None, None]
    cos, sin = jnp.cos(angle), jnp.sin(angle) * sign
    grouped = mixer_input.reshape(rows, groups, width)
    drive = jnp.einsum("tgh,kpgnh->kpgtn", grouped, input_map, preferred_element_type=jnp.float32)
    drive = drive * jnp.sqrt(-jnp.expm1(-time_step))[:, None, :, None, None]
    rotated = jnp.concatenate(
        (cos * drive[:, 0] + sin * drive[:, 1], cos * drive[:, 1] - sin * drive[:, 0]), axis=3
    )
    local = jnp.einsum("kgts,kgsn->kgtn", weights, rotated, precision=highest)
    ends = jnp.stack((local[0, :, -1], local[1, :, 0]))
    totals = jnp.stack((log_sum[0, :, -1], log_sum[1, :, 0]))
    flat = ends.reshape(2 * groups, 2 * states)
    spare = jnp.pad(totals.reshape(1, 2 * groups), ((0, 7), (0, 2 * states - 2 * groups)))
    every = gather_ends(jnp.concatenate((flat, spare), axis=0), count)
    end_all = every[:, : 2 * groups].reshape(count, 2, groups, 2 * states)
    total_all = every[:, 2 * groups, : 2 * groups].reshape(count, 2, groups)
    index = jnp.arange(count)
    away = jnp.stack((mine - index, index - mine), axis=1)
    lo = jnp.minimum(index, mine)[:, None]
    hi = jnp.maximum(index, mine)[:, None]
    between = ((index[None, :] > lo) & (index[None, :] < hi)).astype(jnp.float32)
    span = jnp.einsum("ji,ikg->jkg", between, total_all, precision=highest)
    factor = jnp.where(away[:, :, None] > 0, jnp.exp(span), 0.0)
    block_turn = turns(time_step[:, :, None], number * rows)
    hop = jnp.abs(mine - index).astype(jnp.float32)[:, None, None, None] * block_turn
    hop = math.pi * (hop - 2.0 * jnp.floor(hop * 0.5))
    hop_cos, hop_sin = jnp.cos(hop) * factor[..., None], jnp.sin(hop) * factor[..., None]
    end_re, end_im = end_all[..., :states], end_all[..., states:]
    carry = jnp.concatenate(
        (
            jnp.sum(hop_cos * end_re - hop_sin * end_im, axis=0),
            jnp.sum(hop_cos * end_im + hop_sin * end_re, axis=0),
        ),
        axis=2,
    )
    local = local + jnp.exp(log_sum)[..., None] * carry[:, :, None, :]
    re, im = local[..., :states], local[..., states:]
    state = jnp.concatenate((cos * re - sin * im, cos * im + sin * re), axis=3)
    out_map = jnp.concatenate((readout[:, 0], -readout[:, 1]), axis=3)
    mixed = jnp.einsum("kgtn,kghn->tgh", state, out_map, precision=highest)
    return mixed.reshape(rows, groups * width) + skip_gain[None, :] * mixer_input.astype(
        jnp.float32
    )


def spread(blocks):
    count, mine = lax.axis_size("sp"), lax.axis_index("sp")
    result = jnp.zeros_like(blocks)
    for offset in range(count):
        piece = lax.dynamic_index_in_dim(blocks, (mine + offset) % count, 0, keepdims=True)
        if offset:
            piece = lax.ppermute(piece, "sp", [(i, (i + offset) % count) for i in range(count)])
        result = lax.dynamic_update_slice_in_dim(result, piece, (mine - offset) % count, 0)
    return result


def body(
    mixer_input,
    time_step,
    damping,
    input_map,
    readout,
    skip_gain,
    out_gain,
    out_weight,
    residual,
    channel_gain,
    value_weight,
    gate_weight,
    value_taps,
    gate_taps,
    down_weight,
):
    count, mine = lax.axis_size("sp"), lax.axis_index("sp")
    depth, hidden_width = value_weight.shape
    part = hidden_width // count
    up_send = jnp.concatenate(
        (
            value_weight.reshape(depth, count, part).swapaxes(0, 1),
            gate_weight.reshape(depth, count, part).swapaxes(0, 1),
        ),
        axis=2,
    )
    down_send = down_weight.reshape(count, part, down_weight.shape[1])
    up_all = spread(up_send).reshape(count * depth, 2 * part)
    down_all = spread(down_send).swapaxes(0, 1).reshape(part, count * down_weight.shape[1])
    mixed_y = mixer(mixer_input, time_step, damping, input_map, readout, skip_gain)
    tp_count = lax.axis_size("tp")
    mixed_y = mixed_y.reshape(tp_count, -1, out_gain.shape[0])
    gain_row = jnp.broadcast_to(out_gain, (tp_count, 1, out_gain.shape[0]))
    mixed_y = jnp.concatenate((mixed_y, gain_row), axis=1)
    mixed_y = lax.all_to_all(mixed_y, "tp", split_axis=0, concat_axis=0, tiled=True)
    mixed_y = mixed_y.swapaxes(0, 1).reshape(mixed_y.shape[1], -1)
    mixed_y, gain = mixed_y[:-1], mixed_y[-1]
    inverse = lax.rsqrt(jnp.mean(mixed_y * mixed_y, axis=1, keepdims=True) + norm_eps)
    normed_mix = (mixed_y * inverse * gain[None, :]).astype(jnp.bfloat16)
    mixed_rows = jnp.dot(normed_mix, out_weight, preferred_element_type=jnp.float32)
    hidden_state = (residual.astype(jnp.float32) + mixed_rows).astype(jnp.bfloat16)
    state_wide = hidden_state.astype(jnp.float32)
    scale_rows = lax.rsqrt(jnp.mean(state_wide * state_wide, axis=1, keepdims=True) + norm_eps)
    normed = (state_wide * scale_rows * channel_gain[None, :]).astype(jnp.bfloat16)
    taps = jnp.concatenate(
        (
            lax.dynamic_slice_in_dim(value_taps, mine * part, part, axis=1),
            lax.dynamic_slice_in_dim(gate_taps, mine * part, part, axis=1),
        ),
        axis=1,
    )
    return channel_mixer(normed, hidden_state, up_all, down_all, taps, count, tp_count)


def solution(mesh):
    in_specs = (
        P("sp", "tp"),
        P(None, "tp"),
        P(None, "sp", "tp"),
        P(None, None, "tp", None, None),
        P(None, None, "tp", None, None),
        P("tp"),
        P("tp"),
        P(),
        P(("sp", "tp"), None),
        P(),
        P("sp", "tp"),
        P("sp", "tp"),
        P(None, "tp"),
        P(None, "tp"),
        P("tp", "sp"),
    )
    out_specs = P(("sp", "tp"), None)
    return jax.shard_map(body, mesh=mesh, in_specs=in_specs, out_specs=out_specs, check_vma=False)
```

```python
import math

import jax
import jax.numpy as jnp
from jax import lax
from jax.experimental import pallas as pl
from jax.experimental.pallas import tpu as pltpu
from jax.sharding import PartitionSpec as P

norm_eps = 1e-06
highest = lax.Precision.HIGHEST
mesh_ids = pl.DeviceIdType.MESH


def carry_kernel(count, own_ref, all_ref, local_sem, send_sem, recv_sem):
    sp, tp = lax.axis_index("sp"), lax.axis_index("tp")
    barrier = pltpu.get_barrier_semaphore()
    for offset in range(1, count):
        peer = lax.rem(sp + offset, count)
        pl.semaphore_signal(barrier, inc=1, device_id=(peer, tp), device_id_type=mesh_ids)
    pl.semaphore_wait(barrier, count - 1)
    keep = pltpu.make_async_copy(own_ref, all_ref.at[sp], local_sem)
    keep.start()
    copies = []
    for offset in range(1, count):
        peer = lax.rem(sp + offset, count)
        copy = pltpu.make_async_remote_copy(
            src_ref=own_ref,
            dst_ref=all_ref.at[sp],
            send_sem=send_sem.at[offset],
            recv_sem=recv_sem.at[offset],
            device_id=(peer, tp),
            device_id_type=mesh_ids,
        )
        copy.start()
        copies.append(copy)
    keep.wait()
    for copy in copies:
        copy.wait()


def gather_ends(packed, count):
    vmem = pl.BlockSpec(memory_space=pltpu.VMEM)
    return pl.pallas_call(
        lambda *refs: carry_kernel(count, *refs),
        name="gather_ends",
        out_shape=jax.ShapeDtypeStruct((count,) + packed.shape, packed.dtype),
        in_specs=[vmem],
        out_specs=vmem,
        scratch_shapes=[
            pltpu.SemaphoreType.DMA,
            pltpu.SemaphoreType.DMA((count,)),
            pltpu.SemaphoreType.DMA((count,)),
        ],
        compiler_params=pltpu.CompilerParams(collective_id=0, has_side_effects=True),
    )(packed)


gather_orders = (("z", "y", "x", "c"), ("y", "z", "x", "c"))
sum_orders = (("c", "x", "y", "z"), ("c", "z", "y", "x"))
axes = ("z", "y", "x", "c")


def channel_kernel(sizes, *refs):
    normed_ref, hidden_state_ref, up_send, down_send, taps_ref, out_ref = refs[:6]
    rows_all, up_rows, partial, up_land, down_land, down_ref = refs[6:12]
    landing = refs[12:20]
    local_sem, send_sem, recv_sem, weight_send_sem, weight_recv_sem = refs[20:25]
    rows, width = normed_ref.shape
    half = width // 2
    count, part, part_width = down_send.shape
    sp, tp = lax.axis_index("sp"), lax.axis_index("tp")
    mine = {
        "z": sp // sizes["y"],
        "y": lax.rem(sp, sizes["y"]),
        "x": tp // sizes["c"],
        "c": lax.rem(tp, sizes["c"]),
    }

    def neighbour(axis, offset):
        at = dict(mine)
        at[axis] = lax.rem(mine[axis] + offset, sizes[axis])
        return at[axis], (at["z"] * sizes["y"] + at["y"], at["x"] * sizes["c"] + at["c"])

    barrier = pltpu.get_barrier_semaphore()
    greeted = 0
    for axis in ("x", "c"):
        for offset in range(1, sizes[axis]):
            _, device = neighbour(axis, offset)
            pl.semaphore_signal(barrier, inc=1, device_id=device, device_id_type=mesh_ids)
            greeted += 1
    for offset in range(1, count):
        peer = lax.rem(sp + offset, count)
        pl.semaphore_signal(barrier, inc=1, device_id=(peer, tp), device_id_type=mesh_ids)
        greeted += 1
    pl.semaphore_wait(barrier, greeted)

    keeps = []
    for kind, (source, target) in enumerate(
        (
            (normed_ref, rows_all.at[mine["z"], mine["y"], mine["x"], mine["c"]]),
            (up_send.at[sp], up_land.at[sp]),
            (down_send.at[sp], down_land.at[sp]),
        )
    ):
        keep = pltpu.make_async_copy(source, target, local_sem.at[kind])
        keep.start()
        keeps.append(keep)
    keeps[0].wait()

    def spread(source, land, kind):
        started = []
        for offset in range(1, count):
            peer = lax.rem(sp + offset, count)
            copy = pltpu.make_async_remote_copy(
                src_ref=source.at[peer],
                dst_ref=land.at[sp],
                send_sem=weight_send_sem.at[kind, offset],
                recv_sem=weight_recv_sem.at[kind, offset],
                device_id=(peer, tp),
                device_id_type=mesh_ids,
            )
            copy.start()
            started.append(copy)
        return started

    slot = 0
    pending = [[], []]
    up_copies, down_copies = [], []
    for stage in range(4):
        if stage == 2:
            up_copies = spread(up_send, up_land, 0)
            down_copies = spread(down_send, down_land, 1)
        for piece in range(2):
            axis = gather_orders[piece][stage]
            done = gather_orders[piece][:stage]
            for copy in pending[piece]:
                copy.wait()
            pending[piece] = []
            index = tuple(slice(None) if name in done else mine[name] for name in axes)
            block = rows_all.at[index + (slice(None), pl.ds(piece * half, half))]
            for offset in range(1, sizes[axis]):
                _, device = neighbour(axis, offset)
                copy = pltpu.make_async_remote_copy(
                    src_ref=block,
                    dst_ref=block,
                    send_sem=send_sem.at[slot],
                    recv_sem=recv_sem.at[slot],
                    device_id=device,
                    device_id_type=mesh_ids,
                )
                copy.start()
                pending[piece].append(copy)
                slot += 1
    for piece in range(2):
        for copy in pending[piece]:
            copy.wait()

    plane = sizes["y"] * sizes["x"] * sizes["c"] * rows
    total = plane * sizes["z"]
    for copy in [keeps[1]] + up_copies:
        copy.wait()
    edge = jnp.zeros((8, up_rows.shape[1]), jnp.float32)
    up_rows[pl.ds(0, 8), :] = edge
    up_rows[pl.ds(total + 8, 8), :] = edge

    def project(z, _):
        block = rows_all[z].reshape(plane, width)
        up_weight = up_land[...].reshape(width, 2 * part)
        up = jnp.dot(block, up_weight, preferred_element_type=jnp.float32)
        start = pl.multiple_of(z * plane + 8, 8)
        up_rows[pl.ds(start, plane), :] = up.astype(jnp.bfloat16).astype(jnp.float32)
        return _

    lax.fori_loop(0, sizes["z"], project, 0)

    for copy in [keeps[2]] + down_copies:
        copy.wait()
    for source in range(count):
        down_ref[:, source * part_width : (source + 1) * part_width] = down_land[source]

    def mix(z, _):
        start = pl.multiple_of(z * plane, 8)
        window = up_rows[pl.ds(start, plane + 16), :]
        convolved = (
            taps_ref[0:1, :] * window[7 : plane + 7]
            + taps_ref[1:2, :] * window[8 : plane + 8]
            + taps_ref[2:3, :] * window[9 : plane + 9]
        )
        gate = convolved[:, part:]
        hidden = convolved[:, :part] * (gate / (1.0 + jnp.exp(-gate)))
        sums = jnp.dot(
            hidden.astype(jnp.bfloat16), down_ref[...], preferred_element_type=jnp.float32
        )
        partial[z] = sums.astype(jnp.bfloat16).reshape(partial.shape[1:])
        return _

    lax.fori_loop(0, sizes["z"], mix, 0)

    def start_sum(piece, stage, slot):
        axis = sum_orders[piece][stage]
        done = sum_orders[piece][:stage]
        started = []
        for offset in range(1, sizes[axis]):
            place, device = neighbour(axis, offset)
            index = tuple(
                place if name == axis else mine[name] if name in done else slice(None)
                for name in axes
            )
            copy = pltpu.make_async_remote_copy(
                src_ref=partial.at[index + (slice(None), pl.ds(piece * half, half))],
                dst_ref=landing[piece * 4 + stage].at[offset - 1],
                send_sem=send_sem.at[slot],
                recv_sem=recv_sem.at[slot],
                device_id=device,
                device_id_type=mesh_ids,
            )
            copy.start()
            started.append(copy)
            slot += 1
        return started, slot

    def add_landed(piece, stage):
        axis = sum_orders[piece][stage]
        done = sum_orders[piece][: stage + 1]
        land = landing[piece * 4 + stage]
        columns = pl.ds(piece * half, half)
        free = [name for name in axes if name not in done]

        def add(step, _):
            index, inner = [], ()
            for name in axes:
                if name in done:
                    index.append(mine[name])
                elif name == free[0]:
                    index.append(step)
                    inner = (step,)
                else:
                    index.append(slice(None))
            index = tuple(index) + (slice(None), columns)
            value = partial[index].astype(jnp.float32)
            for offset in range(1, sizes[axis]):
                value = value + land[(offset - 1,) + inner].astype(jnp.float32)
            if free:
                partial[index] = value.astype(jnp.bfloat16)
            else:
                out_ref[:, columns] = (
                    hidden_state_ref[:, columns].astype(jnp.float32) + value
                ).astype(jnp.bfloat16)
            return _

        if free:
            lax.fori_loop(0, sizes[free[0]], add, 0)
        else:
            add(0, 0)

    slot = send_sem.shape[0] // 2
    for stage in range(4):
        for piece in range(2):
            if stage:
                for copy in pending[piece]:
                    copy.wait()
                add_landed(piece, stage - 1)
            pending[piece], slot = start_sum(piece, stage, slot)
    for piece in range(2):
        for copy in pending[piece]:
            copy.wait()
        add_landed(piece, 3)


def channel_mixer(normed, hidden_state, up_send, down_send, taps, sp_count, tp_count):
    cores = 2
    across = tp_count // cores
    deep = math.gcd(across, sp_count)
    sizes = {"z": sp_count // deep, "y": deep, "x": across, "c": cores}
    rows, width = normed.shape
    half = width // 2
    grid = tuple(sizes[name] for name in axes)
    total = math.prod(grid) * rows
    landing = []
    for order in sum_orders:
        for stage in range(4):
            axis = order[stage]
            left = tuple(sizes[name] for name in axes if name not in order[: stage + 1])
            landing.append(
                pltpu.VMEM((max(sizes[axis] - 1, 1),) + left + (rows, half), jnp.bfloat16)
            )
    copies = 2 * 2 * sum(max(sizes[name] - 1, 0) for name in axes)
    vmem = pl.BlockSpec(memory_space=pltpu.VMEM)
    return pl.pallas_call(
        lambda *refs: channel_kernel(sizes, *refs),
        name="channel_mixer",
        out_shape=jax.ShapeDtypeStruct((rows, width), jnp.bfloat16),
        in_specs=[vmem] * 5,
        out_specs=vmem,
        scratch_shapes=[
            pltpu.VMEM(grid + (rows, width), jnp.bfloat16),
            pltpu.VMEM((total + 16, up_send.shape[2]), jnp.float32),
            pltpu.VMEM(grid + (rows, width), jnp.bfloat16),
            pltpu.VMEM(up_send.shape, jnp.bfloat16),
            pltpu.VMEM(down_send.shape, jnp.bfloat16),
            pltpu.VMEM((down_send.shape[1], width), jnp.bfloat16),
            *landing,
            pltpu.SemaphoreType.DMA((3,)),
            pltpu.SemaphoreType.DMA((copies,)),
            pltpu.SemaphoreType.DMA((copies,)),
            pltpu.SemaphoreType.DMA((2, sp_count)),
            pltpu.SemaphoreType.DMA((2, sp_count)),
        ],
        compiler_params=pltpu.CompilerParams(
            collective_id=1, has_side_effects=True, vmem_limit_bytes=63 * 1024 * 1024
        ),
    )(normed, hidden_state, up_send, down_send, taps)


def turns(step_size, count):
    coarse = jnp.round(step_size * 1024.0) / 1024.0
    whole = coarse * count
    whole = whole - 2.0 * jnp.floor(whole * 0.5)
    return whole + (step_size - coarse) * count


def mixer(mixer_input, time_step, damping, input_map, readout, skip_gain):
    rows = mixer_input.shape[0]
    groups = time_step.shape[1]
    states, width = input_map.shape[3], input_map.shape[4]
    count, mine = lax.axis_size("sp"), lax.axis_index("sp")
    at = jnp.arange(rows)
    lower = at[:, None] >= at[None, :]
    reach = jnp.stack((lower, lower.T))
    log_decay = -0.5 * time_step[:, None, :] - damping
    log_sum = jnp.einsum("ktu,kug->kgt", reach.astype(jnp.float32), log_decay, precision=highest)
    weights = jnp.where(
        reach[:, None],
        jnp.exp(jnp.minimum(log_sum[:, :, :, None] - log_sum[:, :, None, :], 0.0)),
        0.0,
    )
    number = jnp.arange(states, dtype=jnp.float32)
    dt = time_step[:, :, None, None]
    angle = math.pi * turns(dt, number[None, :] * at.astype(jnp.float32)[:, None])
    sign = jnp.array([1.0, -1.0], jnp.float32)[:, None, None, None]
    cos, sin = jnp.cos(angle), jnp.sin(angle) * sign
    grouped = mixer_input.reshape(rows, groups, width)
    drive = jnp.einsum("tgh,kpgnh->kpgtn", grouped, input_map, preferred_element_type=jnp.float32)
    drive = drive * jnp.sqrt(-jnp.expm1(-time_step))[:, None, :, None, None]
    rotated = jnp.concatenate(
        (cos * drive[:, 0] + sin * drive[:, 1], cos * drive[:, 1] - sin * drive[:, 0]), axis=3
    )
    local = jnp.einsum("kgts,kgsn->kgtn", weights, rotated, precision=highest)
    ends = jnp.stack((local[0, :, -1], local[1, :, 0]))
    totals = jnp.stack((log_sum[0, :, -1], log_sum[1, :, 0]))
    flat = ends.reshape(2 * groups, 2 * states)
    spare = jnp.pad(totals.reshape(1, 2 * groups), ((0, 7), (0, 2 * states - 2 * groups)))
    every = gather_ends(jnp.concatenate((flat, spare), axis=0), count)
    end_all = every[:, : 2 * groups].reshape(count, 2, groups, 2 * states)
    total_all = every[:, 2 * groups, : 2 * groups].reshape(count, 2, groups)
    index = jnp.arange(count)
    away = jnp.stack((mine - index, index - mine), axis=1)
    lo = jnp.minimum(index, mine)[:, None]
    hi = jnp.maximum(index, mine)[:, None]
    between = ((index[None, :] > lo) & (index[None, :] < hi)).astype(jnp.float32)
    span = jnp.einsum("ji,ikg->jkg", between, total_all, precision=highest)
    factor = jnp.where(away[:, :, None] > 0, jnp.exp(span), 0.0)
    block_turn = turns(time_step[:, :, None], number * rows)
    hop = jnp.abs(mine - index).astype(jnp.float32)[:, None, None, None] * block_turn
    hop = math.pi * (hop - 2.0 * jnp.floor(hop * 0.5))
    hop_cos, hop_sin = jnp.cos(hop) * factor[..., None], jnp.sin(hop) * factor[..., None]
    end_re, end_im = end_all[..., :states], end_all[..., states:]
    carry = jnp.concatenate(
        (
            jnp.sum(hop_cos * end_re - hop_sin * end_im, axis=0),
            jnp.sum(hop_cos * end_im + hop_sin * end_re, axis=0),
        ),
        axis=2,
    )
    local = local + jnp.exp(log_sum)[..., None] * carry[:, :, None, :]
    re, im = local[..., :states], local[..., states:]
    state = jnp.concatenate((cos * re - sin * im, cos * im + sin * re), axis=3)
    out_map = jnp.concatenate((readout[:, 0], -readout[:, 1]), axis=3)
    mixed = jnp.einsum("kgtn,kghn->tgh", state, out_map, precision=highest)
    return mixed.reshape(rows, groups * width) + skip_gain[None, :] * mixer_input.astype(
        jnp.float32
    )


def body(
    mixer_input,
    time_step,
    damping,
    input_map,
    readout,
    skip_gain,
    out_gain,
    out_weight,
    residual,
    channel_gain,
    value_weight,
    gate_weight,
    value_taps,
    gate_taps,
    down_weight,
):
    count, mine = lax.axis_size("sp"), lax.axis_index("sp")
    depth, hidden_width = value_weight.shape
    part = hidden_width // count
    up_send = jnp.concatenate(
        (
            value_weight.reshape(depth, count, part).swapaxes(0, 1),
            gate_weight.reshape(depth, count, part).swapaxes(0, 1),
        ),
        axis=2,
    )
    down_send = down_weight.reshape(count, part, down_weight.shape[1])
    mixed_y = mixer(mixer_input, time_step, damping, input_map, readout, skip_gain)
    tp_count = lax.axis_size("tp")
    mixed_y = mixed_y.reshape(tp_count, -1, out_gain.shape[0])
    gain_row = jnp.broadcast_to(out_gain, (tp_count, 1, out_gain.shape[0]))
    mixed_y = jnp.concatenate((mixed_y, gain_row), axis=1)
    mixed_y = lax.all_to_all(mixed_y, "tp", split_axis=0, concat_axis=0, tiled=True)
    mixed_y = mixed_y.swapaxes(0, 1).reshape(mixed_y.shape[1], -1)
    mixed_y, gain = mixed_y[:-1], mixed_y[-1]
    inverse = lax.rsqrt(jnp.mean(mixed_y * mixed_y, axis=1, keepdims=True) + norm_eps)
    normed_mix = (mixed_y * inverse * gain[None, :]).astype(jnp.bfloat16)
    mixed_rows = jnp.dot(normed_mix, out_weight, preferred_element_type=jnp.float32)
    hidden_state = (residual.astype(jnp.float32) + mixed_rows).astype(jnp.bfloat16)
    state_wide = hidden_state.astype(jnp.float32)
    scale_rows = lax.rsqrt(jnp.mean(state_wide * state_wide, axis=1, keepdims=True) + norm_eps)
    normed = (state_wide * scale_rows * channel_gain[None, :]).astype(jnp.bfloat16)
    taps = jnp.concatenate(
        (
            lax.dynamic_slice_in_dim(value_taps, mine * part, part, axis=1),
            lax.dynamic_slice_in_dim(gate_taps, mine * part, part, axis=1),
        ),
        axis=1,
    )
    return channel_mixer(normed, hidden_state, up_send, down_send, taps, count, tp_count)


def solution(mesh):
    in_specs = (
        P("sp", "tp"),
        P(None, "tp"),
        P(None, "sp", "tp"),
        P(None, None, "tp", None, None),
        P(None, None, "tp", None, None),
        P("tp"),
        P("tp"),
        P(),
        P(("sp", "tp"), None),
        P(),
        P("sp", "tp"),
        P("sp", "tp"),
        P(None, "tp"),
        P(None, "tp"),
        P("tp", "sp"),
    )
    out_specs = P(("sp", "tp"), None)
    return jax.shard_map(body, mesh=mesh, in_specs=in_specs, out_specs=out_specs, check_vma=False)
```

```python
import math

import jax
import jax.numpy as jnp
from jax import lax
from jax.experimental import pallas as pl
from jax.experimental.pallas import tpu as pltpu
from jax.sharding import PartitionSpec as P

norm_eps = 1e-06
highest = lax.Precision.HIGHEST
mesh_ids = pl.DeviceIdType.MESH


def carry_kernel(count, own_ref, all_ref, local_sem, send_sem, recv_sem):
    sp, tp = lax.axis_index("sp"), lax.axis_index("tp")
    barrier = pltpu.get_barrier_semaphore()
    for offset in range(1, count):
        peer = lax.rem(sp + offset, count)
        pl.semaphore_signal(barrier, inc=1, device_id=(peer, tp), device_id_type=mesh_ids)
    pl.semaphore_wait(barrier, count - 1)
    keep = pltpu.make_async_copy(own_ref, all_ref.at[sp], local_sem)
    keep.start()
    copies = []
    for offset in range(1, count):
        peer = lax.rem(sp + offset, count)
        copy = pltpu.make_async_remote_copy(
            src_ref=own_ref,
            dst_ref=all_ref.at[sp],
            send_sem=send_sem.at[offset],
            recv_sem=recv_sem.at[offset],
            device_id=(peer, tp),
            device_id_type=mesh_ids,
        )
        copy.start()
        copies.append(copy)
    keep.wait()
    for copy in copies:
        copy.wait()


def gather_ends(packed, count):
    vmem = pl.BlockSpec(memory_space=pltpu.VMEM)
    return pl.pallas_call(
        lambda *refs: carry_kernel(count, *refs),
        name="gather_ends",
        out_shape=jax.ShapeDtypeStruct((count,) + packed.shape, packed.dtype),
        in_specs=[vmem],
        out_specs=vmem,
        scratch_shapes=[
            pltpu.SemaphoreType.DMA,
            pltpu.SemaphoreType.DMA((count,)),
            pltpu.SemaphoreType.DMA((count,)),
        ],
        compiler_params=pltpu.CompilerParams(collective_id=0, has_side_effects=True),
    )(packed)


gather_orders = (("z", "y", "x", "c"), ("y", "z", "x", "c"))
sum_orders = (("c", "x", "y", "z"), ("c", "z", "y", "x"))
axes = ("z", "y", "x", "c")


def channel_kernel(sizes, *refs):
    normed_ref, hidden_state_ref, up_send, down_send, taps_ref, out_ref = refs[:6]
    rows_all, up_rows, partial, up_land, down_land, down_ref = refs[6:12]
    landing = refs[12:20]
    local_sem, send_sem, recv_sem, weight_send_sem, weight_recv_sem = refs[20:25]
    rows, width = normed_ref.shape
    half = width // 2
    count, part, part_width = down_send.shape
    sp, tp = lax.axis_index("sp"), lax.axis_index("tp")
    mine = {
        "z": sp // sizes["y"],
        "y": lax.rem(sp, sizes["y"]),
        "x": tp // sizes["c"],
        "c": lax.rem(tp, sizes["c"]),
    }

    def neighbour(axis, offset):
        at = dict(mine)
        at[axis] = lax.rem(mine[axis] + offset, sizes[axis])
        return at[axis], (at["z"] * sizes["y"] + at["y"], at["x"] * sizes["c"] + at["c"])

    barrier = pltpu.get_barrier_semaphore()
    greeted = 0
    for axis in ("x", "c"):
        for offset in range(1, sizes[axis]):
            _, device = neighbour(axis, offset)
            pl.semaphore_signal(barrier, inc=1, device_id=device, device_id_type=mesh_ids)
            greeted += 1
    for offset in range(1, count):
        peer = lax.rem(sp + offset, count)
        pl.semaphore_signal(barrier, inc=1, device_id=(peer, tp), device_id_type=mesh_ids)
        greeted += 1
    pl.semaphore_wait(barrier, greeted)

    keeps = []
    for kind, (source, target) in enumerate(
        (
            (normed_ref, rows_all.at[mine["z"], mine["y"], mine["x"], mine["c"]]),
            (up_send.at[sp], up_land.at[sp]),
            (down_send.at[sp], down_land.at[sp]),
        )
    ):
        keep = pltpu.make_async_copy(source, target, local_sem.at[kind])
        keep.start()
        keeps.append(keep)
    keeps[0].wait()

    def spread(source, land, kind):
        started = []
        for offset in range(1, count):
            peer = lax.rem(sp + offset, count)
            copy = pltpu.make_async_remote_copy(
                src_ref=source.at[peer],
                dst_ref=land.at[sp],
                send_sem=weight_send_sem.at[kind, offset],
                recv_sem=weight_recv_sem.at[kind, offset],
                device_id=(peer, tp),
                device_id_type=mesh_ids,
            )
            copy.start()
            started.append(copy)
        return started

    slot = 0
    pending = [[], []]
    up_copies, down_copies = [], []
    for stage in range(4):
        if stage == 2:
            up_copies = spread(up_send, up_land, 0)
            down_copies = spread(down_send, down_land, 1)
        for piece in range(2):
            axis = gather_orders[piece][stage]
            done = gather_orders[piece][:stage]
            for copy in pending[piece]:
                copy.wait()
            pending[piece] = []
            index = tuple(slice(None) if name in done else mine[name] for name in axes)
            block = rows_all.at[index + (slice(None), pl.ds(piece * half, half))]
            for offset in range(1, sizes[axis]):
                _, device = neighbour(axis, offset)
                copy = pltpu.make_async_remote_copy(
                    src_ref=block,
                    dst_ref=block,
                    send_sem=send_sem.at[slot],
                    recv_sem=recv_sem.at[slot],
                    device_id=device,
                    device_id_type=mesh_ids,
                )
                copy.start()
                pending[piece].append(copy)
                slot += 1
    for piece in range(2):
        for copy in pending[piece]:
            copy.wait()

    plane = sizes["y"] * sizes["x"] * sizes["c"] * rows
    total = plane * sizes["z"]
    for copy in [keeps[1]] + up_copies:
        copy.wait()
    edge = jnp.zeros((8, up_rows.shape[1]), jnp.float32)
    up_rows[pl.ds(0, 8), :] = edge
    up_rows[pl.ds(total + 8, 8), :] = edge

    def project(z, _):
        block = rows_all[z].reshape(plane, width)
        up_weight = up_land[...].reshape(width, 2 * part)
        up = jnp.dot(block, up_weight, preferred_element_type=jnp.float32)
        start = pl.multiple_of(z * plane + 8, 8)
        up_rows[pl.ds(start, plane), :] = up.astype(jnp.bfloat16).astype(jnp.float32)
        return _

    lax.fori_loop(0, sizes["z"], project, 0)

    for copy in [keeps[2]] + down_copies:
        copy.wait()
    for source in range(count):
        down_ref[:, source * part_width : (source + 1) * part_width] = down_land[source]

    def mix(z, _):
        start = pl.multiple_of(z * plane, 8)
        window = up_rows[pl.ds(start, plane + 16), :]
        convolved = (
            taps_ref[0:1, :] * window[7 : plane + 7]
            + taps_ref[1:2, :] * window[8 : plane + 8]
            + taps_ref[2:3, :] * window[9 : plane + 9]
        )
        gate = convolved[:, part:]
        hidden = convolved[:, :part] * (gate / (1.0 + jnp.exp(-gate)))
        sums = jnp.dot(
            hidden.astype(jnp.bfloat16), down_ref[...], preferred_element_type=jnp.float32
        )
        partial[z] = sums.astype(jnp.bfloat16).reshape(partial.shape[1:])
        return _

    lax.fori_loop(0, sizes["z"], mix, 0)

    def start_sum(piece, stage, slot):
        axis = sum_orders[piece][stage]
        done = sum_orders[piece][:stage]
        started = []
        for offset in range(1, sizes[axis]):
            place, device = neighbour(axis, offset)
            index = tuple(
                place if name == axis else mine[name] if name in done else slice(None)
                for name in axes
            )
            copy = pltpu.make_async_remote_copy(
                src_ref=partial.at[index + (slice(None), pl.ds(piece * half, half))],
                dst_ref=landing[piece * 4 + stage].at[offset - 1],
                send_sem=send_sem.at[slot],
                recv_sem=recv_sem.at[slot],
                device_id=device,
                device_id_type=mesh_ids,
            )
            copy.start()
            started.append(copy)
            slot += 1
        return started, slot

    def add_landed(piece, stage):
        axis = sum_orders[piece][stage]
        done = sum_orders[piece][: stage + 1]
        land = landing[piece * 4 + stage]
        columns = pl.ds(piece * half, half)
        free = [name for name in axes if name not in done]

        def add(step, _):
            index, inner = [], ()
            for name in axes:
                if name in done:
                    index.append(mine[name])
                elif name == free[0]:
                    index.append(step)
                    inner = (step,)
                else:
                    index.append(slice(None))
            index = tuple(index) + (slice(None), columns)
            value = partial[index].astype(jnp.float32)
            for offset in range(1, sizes[axis]):
                value = value + land[(offset - 1,) + inner].astype(jnp.float32)
            if free:
                partial[index] = value.astype(jnp.bfloat16)
            else:
                out_ref[:, columns] = (
                    hidden_state_ref[:, columns].astype(jnp.float32) + value
                ).astype(jnp.bfloat16)
            return _

        if free:
            lax.fori_loop(0, sizes[free[0]], add, 0)
        else:
            add(0, 0)

    slot = send_sem.shape[0] // 2
    for stage in range(4):
        for piece in range(2):
            if stage:
                for copy in pending[piece]:
                    copy.wait()
                add_landed(piece, stage - 1)
            pending[piece], slot = start_sum(piece, stage, slot)
    for piece in range(2):
        for copy in pending[piece]:
            copy.wait()
        add_landed(piece, 3)


def channel_mixer(normed, hidden_state, up_send, down_send, taps, sp_count, tp_count):
    cores = 2
    across = tp_count // cores
    deep = math.gcd(across, sp_count)
    sizes = {"z": sp_count // deep, "y": deep, "x": across, "c": cores}
    rows, width = normed.shape
    half = width // 2
    grid = tuple(sizes[name] for name in axes)
    total = math.prod(grid) * rows
    landing = []
    for order in sum_orders:
        for stage in range(4):
            axis = order[stage]
            left = tuple(sizes[name] for name in axes if name not in order[: stage + 1])
            landing.append(
                pltpu.VMEM((max(sizes[axis] - 1, 1),) + left + (rows, half), jnp.bfloat16)
            )
    copies = 2 * 2 * sum(max(sizes[name] - 1, 0) for name in axes)
    vmem = pl.BlockSpec(memory_space=pltpu.VMEM)
    return pl.pallas_call(
        lambda *refs: channel_kernel(sizes, *refs),
        name="channel_mixer",
        out_shape=jax.ShapeDtypeStruct((rows, width), jnp.bfloat16),
        in_specs=[vmem] * 5,
        out_specs=vmem,
        scratch_shapes=[
            pltpu.VMEM(grid + (rows, width), jnp.bfloat16),
            pltpu.VMEM((total + 16, up_send.shape[2]), jnp.float32),
            pltpu.VMEM(grid + (rows, width), jnp.bfloat16),
            pltpu.VMEM(up_send.shape, jnp.bfloat16),
            pltpu.VMEM(down_send.shape, jnp.bfloat16),
            pltpu.VMEM((down_send.shape[1], width), jnp.bfloat16),
            *landing,
            pltpu.SemaphoreType.DMA((3,)),
            pltpu.SemaphoreType.DMA((copies,)),
            pltpu.SemaphoreType.DMA((copies,)),
            pltpu.SemaphoreType.DMA((2, sp_count)),
            pltpu.SemaphoreType.DMA((2, sp_count)),
        ],
        compiler_params=pltpu.CompilerParams(
            collective_id=1, has_side_effects=True, vmem_limit_bytes=63 * 1024 * 1024
        ),
    )(normed, hidden_state, up_send, down_send, taps)


def turns(step_size, count):
    coarse = jnp.round(step_size * 1024.0) / 1024.0
    whole = coarse * count
    whole = whole - 2.0 * jnp.floor(whole * 0.5)
    return whole + (step_size - coarse) * count


def mixer(mixer_input, time_step, damping, input_map, readout, skip_gain):
    rows = mixer_input.shape[0]
    groups = time_step.shape[1]
    states, width = input_map.shape[3], input_map.shape[4]
    count, mine = lax.axis_size("sp"), lax.axis_index("sp")
    at = jnp.arange(rows)
    lower = at[:, None] >= at[None, :]
    reach = jnp.stack((lower, lower.T))
    log_decay = -0.5 * time_step[:, None, :] - damping
    log_sum = jnp.einsum("ktu,kug->kgt", reach.astype(jnp.float32), log_decay, precision=highest)
    weights = jnp.where(
        reach[:, None],
        jnp.exp(jnp.minimum(log_sum[:, :, :, None] - log_sum[:, :, None, :], 0.0)),
        0.0,
    )
    number = jnp.arange(states, dtype=jnp.float32)
    dt = time_step[:, :, None, None]
    angle = math.pi * turns(dt, number[None, :] * at.astype(jnp.float32)[:, None])
    sign = jnp.array([1.0, -1.0], jnp.float32)[:, None, None, None]
    cos, sin = jnp.cos(angle), jnp.sin(angle) * sign
    grouped = mixer_input.reshape(rows, groups, width)
    drive = jnp.einsum("tgh,kpgnh->kpgtn", grouped, input_map, preferred_element_type=jnp.float32)
    drive = drive * jnp.sqrt(-jnp.expm1(-time_step))[:, None, :, None, None]
    rotated = jnp.concatenate(
        (cos * drive[:, 0] + sin * drive[:, 1], cos * drive[:, 1] - sin * drive[:, 0]), axis=3
    )
    local = jnp.einsum("kgts,kgsn->kgtn", weights, rotated, precision=lax.Precision.HIGH)
    ends = jnp.stack((local[0, :, -1], local[1, :, 0]))
    totals = jnp.stack((log_sum[0, :, -1], log_sum[1, :, 0]))
    flat = ends.reshape(2 * groups, 2 * states)
    spare = jnp.pad(totals.reshape(1, 2 * groups), ((0, 7), (0, 2 * states - 2 * groups)))
    every = gather_ends(jnp.concatenate((flat, spare), axis=0), count)
    end_all = every[:, : 2 * groups].reshape(count, 2, groups, 2 * states)
    total_all = every[:, 2 * groups, : 2 * groups].reshape(count, 2, groups)
    index = jnp.arange(count)
    away = jnp.stack((mine - index, index - mine), axis=1)
    lo = jnp.minimum(index, mine)[:, None]
    hi = jnp.maximum(index, mine)[:, None]
    between = ((index[None, :] > lo) & (index[None, :] < hi)).astype(jnp.float32)
    span = jnp.einsum("ji,ikg->jkg", between, total_all, precision=highest)
    factor = jnp.where(away[:, :, None] > 0, jnp.exp(span), 0.0)
    block_turn = turns(time_step[:, :, None], number * rows)
    hop = jnp.abs(mine - index).astype(jnp.float32)[:, None, None, None] * block_turn
    hop = math.pi * (hop - 2.0 * jnp.floor(hop * 0.5))
    hop_cos, hop_sin = jnp.cos(hop) * factor[..., None], jnp.sin(hop) * factor[..., None]
    end_re, end_im = end_all[..., :states], end_all[..., states:]
    carry = jnp.concatenate(
        (
            jnp.sum(hop_cos * end_re - hop_sin * end_im, axis=0),
            jnp.sum(hop_cos * end_im + hop_sin * end_re, axis=0),
        ),
        axis=2,
    )
    local = local + jnp.exp(log_sum)[..., None] * carry[:, :, None, :]
    re, im = local[..., :states], local[..., states:]
    state = jnp.concatenate((cos * re - sin * im, cos * im + sin * re), axis=3)
    out_map = jnp.concatenate((readout[:, 0], -readout[:, 1]), axis=3)
    mixed = jnp.einsum("kgtn,kghn->tgh", state, out_map, precision=lax.Precision.HIGH)
    return mixed.reshape(rows, groups * width) + skip_gain[None, :] * mixer_input.astype(
        jnp.float32
    )


def body(
    mixer_input,
    time_step,
    damping,
    input_map,
    readout,
    skip_gain,
    out_gain,
    out_weight,
    residual,
    channel_gain,
    value_weight,
    gate_weight,
    value_taps,
    gate_taps,
    down_weight,
):
    count, mine = lax.axis_size("sp"), lax.axis_index("sp")
    depth, hidden_width = value_weight.shape
    part = hidden_width // count
    up_send = jnp.concatenate(
        (
            value_weight.reshape(depth, count, part).swapaxes(0, 1),
            gate_weight.reshape(depth, count, part).swapaxes(0, 1),
        ),
        axis=2,
    )
    down_send = down_weight.reshape(count, part, down_weight.shape[1])
    mixed_y = mixer(mixer_input, time_step, damping, input_map, readout, skip_gain)
    tp_count = lax.axis_size("tp")
    mixed_y = mixed_y.reshape(tp_count, -1, out_gain.shape[0])
    gain_row = jnp.broadcast_to(out_gain, (tp_count, 1, out_gain.shape[0]))
    mixed_y = jnp.concatenate((mixed_y, gain_row), axis=1)
    mixed_y = lax.all_to_all(mixed_y, "tp", split_axis=0, concat_axis=0, tiled=True)
    mixed_y = mixed_y.swapaxes(0, 1).reshape(mixed_y.shape[1], -1)
    mixed_y, gain = mixed_y[:-1], mixed_y[-1]
    inverse = lax.rsqrt(jnp.mean(mixed_y * mixed_y, axis=1, keepdims=True) + norm_eps)
    normed_mix = (mixed_y * inverse * gain[None, :]).astype(jnp.bfloat16)
    mixed_rows = jnp.dot(normed_mix, out_weight, preferred_element_type=jnp.float32)
    hidden_state = (residual.astype(jnp.float32) + mixed_rows).astype(jnp.bfloat16)
    state_wide = hidden_state.astype(jnp.float32)
    scale_rows = lax.rsqrt(jnp.mean(state_wide * state_wide, axis=1, keepdims=True) + norm_eps)
    normed = (state_wide * scale_rows * channel_gain[None, :]).astype(jnp.bfloat16)
    taps = jnp.concatenate(
        (
            lax.dynamic_slice_in_dim(value_taps, mine * part, part, axis=1),
            lax.dynamic_slice_in_dim(gate_taps, mine * part, part, axis=1),
        ),
        axis=1,
    )
    return channel_mixer(normed, hidden_state, up_send, down_send, taps, count, tp_count)


def solution(mesh):
    in_specs = (
        P("sp", "tp"),
        P(None, "tp"),
        P(None, "sp", "tp"),
        P(None, None, "tp", None, None),
        P(None, None, "tp", None, None),
        P("tp"),
        P("tp"),
        P(),
        P(("sp", "tp"), None),
        P(),
        P("sp", "tp"),
        P("sp", "tp"),
        P(None, "tp"),
        P(None, "tp"),
        P("tp", "sp"),
    )
    out_specs = P(("sp", "tp"), None)
    return jax.shard_map(body, mesh=mesh, in_specs=in_specs, out_specs=out_specs, check_vma=False)
```
